256 devices in a mesh: sp: 32 (over z, y), tp: 8 (over x, core).
Axes of the slice: x: 4, y: 4, z: 8, core: 2. Of those that a mesh axis runs over, the one named last changes fastest.
Arguments:
- residual: bfloat16 [16384, 2048], P(('sp', 'tp')), may hold values from -6 to 6
- query_major: bfloat16 [16384, 1024], P('sp', 'tp'), may hold values from -160 to 160
- keys_major: bfloat16 [16384, 1024], P('sp', 'tp'), may hold values from -6.5 to 6.5
- values_major: bfloat16 [16384, 1024], P('sp', 'tp'), may hold values from -6 to 6
- query_minor: bfloat16 [16384, 512], P('sp', 'tp'), may hold values from -160 to 160
- keys_minor: bfloat16 [16384, 512], P('sp', 'tp'), may hold values from -6.5 to 6.5
- values_minor: bfloat16 [16384, 512], P('sp', 'tp'), may hold values from -6 to 6
- lambda_major: float32 [8], P('tp'), may hold values from 0.3 to 0.8
- lambda_minor: float32 [8], P('tp'), may hold values from 0.3 to 0.8
- gain_major: float32 [128], replicated, may hold values from 0.1 to 1.9
- gain_minor: float32 [64], replicated, may hold values from 0.1 to 1.9
- output_major: bfloat16 [1024, 2048], P('tp'), may hold values from -0.15625 to 0.15625
- output_minor: bfloat16 [512, 2048], P('tp'), may hold values from -0.15625 to 0.15625
- mixer_gain: float32 [2048], replicated, may hold values from 0.1 to 1.9
- up_weight: bfloat16 [2048, 8192], P('sp', 'tp'), may hold values from -0.125 to 0.125
- down_weight: bfloat16 [8192, 2048], P('tp', 'sp'), may hold values from -0.0625 to 0.0625
Outputs:
- layer_out: bfloat16 [16384, 2048], P(('sp', 'tp'))
The draws below stay inside these ranges and needn't reach their ends.
All inputs are finite; a program needn't handle non-finite values.
Results may differ from the reference program's by a relative error of at most 0.018.
Values may be sent and summed in bfloat16 or wider, within the bound.
No kernel may reach another device: no remote copies, remote signals or barrier semaphores. Data moves between devices by JAX's collectives and lax.ppermute only.
A program may use at most 128 MiB of HBM per device.

```python
import jax
import jax.numpy as jnp
from jax import lax

D_MODEL = 2048
D_FF = 8192
H_MAJOR = 8
DK_MAJOR = 64
H_MINOR = 8
DK_MINOR = 32
DV_MAJOR = 128
DV_MINOR = 64
SEGMENT = 64
TOKENS = 16384
N_TP = 8


def drawn(key, head_count, key_size):
    key_query, key_keys = jax.random.split(key, 2)
    shape = (TOKENS, head_count, 2, key_size)
    queries = jnp.clip(jax.random.normal(key_query, shape, jnp.float32), -5.0, 5.0) * 1.3
    key_rows = jnp.clip(jax.random.normal(key_keys, shape, jnp.float32), -5.0, 5.0) * 1.3
    width_all = head_count * 2 * key_size
    return (queries.reshape(TOKENS, width_all), key_rows.reshape(TOKENS, width_all))


def draw_query_major(key, part):
    return drawn(jax.random.fold_in(key, 1), H_MAJOR, DK_MAJOR)[0].astype(jnp.bfloat16)


def draw_keys_major(key, part):
    return drawn(jax.random.fold_in(key, 1), H_MAJOR, DK_MAJOR)[1].astype(jnp.bfloat16)


def draw_query_minor(key, part):
    return drawn(jax.random.fold_in(key, 2), H_MINOR, DK_MINOR)[0].astype(jnp.bfloat16)


def draw_keys_minor(key, part):
    return drawn(jax.random.fold_in(key, 2), H_MINOR, DK_MINOR)[1].astype(jnp.bfloat16)


def shard_levels(stream_key, dims, cuts, low, high):
    gain, own = 1.0, jax.random.fold_in(stream_key, 6)
    for axis_at, blocks in cuts:
        draws = jnp.exp(jax.random.uniform(jax.random.fold_in(own, axis_at), (blocks,), jnp.float32, low / len(cuts), high / len(cuts)))
        gain = gain * jnp.repeat(draws, dims[axis_at] // blocks).reshape([-1 if axis == axis_at else 1 for axis in range(len(dims))])
    return gain


def normal_values(rng, dims, width, reach, shards=(), kind=jnp.bfloat16):
    gain = shard_levels(rng, dims, shards, -0.22, 0.18) if shards else 1.0
    result = jax.random.normal(rng, dims, jnp.float32) * width * gain
    return jnp.minimum(jnp.maximum(result, -reach), reach).astype(kind)


def setup_inputs(seed: int = 0) -> dict:
    keys = jax.random.split(jax.random.key(seed), 17)
    residual = normal_values(keys[0], (TOKENS, D_MODEL), 1.0, 6.0, ((0, 256),))
    query_major = draw_query_major(jax.random.fold_in(keys[16], 71), 0)
    keys_major = draw_keys_major(jax.random.fold_in(keys[16], 71), 0)
    values_major = normal_values(keys[3], (TOKENS, H_MAJOR * DV_MAJOR), 1.0, 6.0, ((0, 32), (1, 8)))
    query_minor = draw_query_minor(jax.random.fold_in(keys[16], 71), 0)
    keys_minor = draw_keys_minor(jax.random.fold_in(keys[16], 71), 0)
    values_minor = normal_values(keys[6], (TOKENS, H_MINOR * DV_MINOR), 1.0, 6.0, ((0, 32), (1, 8)))
    lambda_major = jnp.clip(0.3 + 0.5 * jax.random.uniform(keys[7], (H_MAJOR,), jnp.float32) ** shard_levels(keys[7], (H_MAJOR,), ((0, 8),), -0.2, 0.2), 0.3, 0.8)
    lambda_minor = jnp.clip(0.3 + 0.5 * jax.random.uniform(keys[8], (H_MINOR,), jnp.float32) ** shard_levels(keys[8], (H_MINOR,), ((0, 8),), -0.2, 0.2), 0.3, 0.8)
    gain_major = jnp.clip(1.0 + 0.18 * jax.random.normal(keys[9], (DV_MAJOR,), jnp.float32), 0.1, 1.9)
    gain_minor = jnp.clip(1.0 + 0.18 * jax.random.normal(keys[10], (DV_MINOR,), jnp.float32), 0.1, 1.9)
    output_major = normal_values(keys[11], (H_MAJOR * DV_MAJOR, D_MODEL), (H_MAJOR * DV_MAJOR + H_MINOR * DV_MINOR) ** -0.5, 0.15625, ((0, 8),))
    output_minor = normal_values(keys[12], (H_MINOR * DV_MINOR, D_MODEL), (H_MAJOR * DV_MAJOR + H_MINOR * DV_MINOR) ** -0.5, 0.15625, ((0, 8),))
    mixer_gain = jnp.clip(1.0 + 0.18 * jax.random.normal(keys[13], (D_MODEL,), jnp.float32), 0.1, 1.9)
    up_weight = normal_values(keys[14], (D_MODEL, D_FF), D_MODEL ** -0.5, 0.125, ((0, 32), (1, 8)))
    down_weight = normal_values(keys[15], (D_FF, D_MODEL), D_FF ** -0.5, 0.0625, ((0, 8), (1, 32)))
    return {"residual": residual, "query_major": query_major, "keys_major": keys_major, "values_major": values_major, "query_minor": query_minor, "keys_minor": keys_minor, "values_minor": values_minor, "lambda_major": lambda_major, "lambda_minor": lambda_minor, "gain_major": gain_major, "gain_minor": gain_minor, "output_major": output_major, "output_minor": output_minor, "mixer_gain": mixer_gain, "up_weight": up_weight, "down_weight": down_weight}


EPSILON = 1e-06

def to_wire(value):
    return lax.optimization_barrier(value.astype(jnp.bfloat16)).astype(jnp.float32)

def head_group(queries, key_rows, values, lambdas, scaling, head_count, key_size):
    value_size = values.shape[1] // head_count
    block_len = 512 if TOKENS % 512 == 0 else TOKENS
    key_pos = jnp.arange(TOKENS, dtype=jnp.int32)
    keys_all = key_rows.astype(jnp.float32).reshape(TOKENS, head_count, 2, key_size)
    values_all = values.astype(jnp.float32).reshape(TOKENS, head_count, value_size)

    def one_block(block_id):
        first_row = (block_id * block_len).astype(jnp.int32)
        query_block = lax.dynamic_slice_in_dim(queries, first_row, block_len, 0).astype(jnp.float32)
        query_block = query_block.reshape(block_len, head_count, 2, key_size)
        query_pos = first_row + jnp.arange(block_len, dtype=jnp.int32)
        visible = key_pos[None, :] // SEGMENT <= query_pos[:, None] // SEGMENT

        def one_head(head_id):
            query_head = lax.dynamic_index_in_dim(query_block, head_id, 1, keepdims=False)
            keys_head = lax.dynamic_index_in_dim(keys_all, head_id, 1, keepdims=False)
            values_head = lax.dynamic_index_in_dim(values_all, head_id, 1, keepdims=False)
            scores = jnp.einsum('qmd,kmd->mqk', query_head, keys_head) * key_size ** (-0.5)
            scores = jnp.where(visible[None], scores, -jnp.inf)
            peak = lax.optimization_barrier(jnp.max(scores, axis=-1, keepdims=True))
            weights = jnp.where(visible[None], jnp.exp(scores - peak), 0.0)
            totals = lax.optimization_barrier(jnp.sum(weights, axis=-1))
            sums = jnp.einsum('mqk,ke->mqe', to_wire(weights), values_head)
            lam_head = lambdas[head_id]
            output = sums[0] / totals[0][:, None] - lam_head * sums[1] / totals[1][:, None]
            output = output * lax.rsqrt(lax.optimization_barrier(jnp.mean(output * output, axis=-1, keepdims=True)) + EPSILON) * scaling
            return output.astype(jnp.bfloat16)
        per_head = lax.map(one_head, jnp.arange(head_count, dtype=jnp.int32))
        return jnp.transpose(per_head, (1, 0, 2)).reshape(block_len, head_count * value_size)
    blocks = lax.map(one_block, jnp.arange(TOKENS // block_len, dtype=jnp.int32))
    return blocks.reshape(TOKENS, head_count * value_size)

def reference(residual, query_major, keys_major, values_major, query_minor, keys_minor, values_minor, lambda_major, lambda_minor, gain_major, gain_minor, output_major, output_minor, mixer_gain, up_weight, down_weight):
    heads_major = head_group(query_major, keys_major, values_major, lambda_major, gain_major, H_MAJOR, DK_MAJOR)
    heads_minor = head_group(query_minor, keys_minor, values_minor, lambda_minor, gain_minor, H_MINOR, DK_MINOR)
    cols_major = H_MAJOR * DV_MAJOR // N_TP
    cols_minor = H_MINOR * DV_MINOR // N_TP
    mixed = jnp.zeros((TOKENS, D_MODEL), jnp.float32)
    for group in range(N_TP):
        partial_sum = jnp.dot(heads_major[:, group * cols_major:(group + 1) * cols_major], output_major[group * cols_major:(group + 1) * cols_major], preferred_element_type=jnp.float32)
        partial_sum = partial_sum + jnp.dot(heads_minor[:, group * cols_minor:(group + 1) * cols_minor], output_minor[group * cols_minor:(group + 1) * cols_minor], preferred_element_type=jnp.float32)
        mixed = mixed + to_wire(partial_sum)
    stream = residual.astype(jnp.float32) + mixed
    normed = stream * lax.rsqrt(lax.optimization_barrier(jnp.mean(stream * stream, axis=-1, keepdims=True)) + EPSILON) * mixer_gain
    normed = normed.astype(jnp.bfloat16)
    hidden = jnp.square(jax.nn.relu(jnp.dot(normed, up_weight, preferred_element_type=jnp.float32)))
    hidden = hidden.astype(jnp.bfloat16)
    cols_ff = D_FF // N_TP
    down_sum = jnp.zeros((TOKENS, D_MODEL), jnp.float32)
    for group in range(N_TP):
        partial_sum = jnp.dot(hidden[:, group * cols_ff:(group + 1) * cols_ff], down_weight[group * cols_ff:(group + 1) * cols_ff], preferred_element_type=jnp.float32)
        down_sum = down_sum + to_wire(partial_sum)
    return (stream + down_sum).astype(jnp.bfloat16)
```

```python
import jax
import jax.numpy as jnp
from jax import lax
from jax.experimental import pallas as pl
from jax.experimental.pallas import tpu as pltpu
from jax.sharding import Mesh
from jax.sharding import PartitionSpec as P

DK_MAJOR = 64
DK_MINOR = 32
SEGMENT = 64
EPSILON = 1e-06
NEGATIVE = -1e30
LOG2E = 1.4426950408889634
SCALES = (DK_MAJOR**-0.5 * LOG2E,) * 2 + (DK_MINOR**-0.5 * LOG2E,) * 2
SP = ("z", "y")
TP = ("x", "c")
ROWS = 416
STATS = 384
NT = (((1,), (1,)), ((), ()))


def dot(a, b, dims=(((1,), (0,)), ((), ()))):
    return lax.dot_general(a, b, dims, preferred_element_type=jnp.float32)


def shifted(value, axis, by):
    size = lax.axis_size(axis)
    return lax.ppermute(value, axis, [(i, (i + by) % size) for i in range(size)])


def mirrored(value):
    size = lax.axis_size("z")
    return lax.ppermute(value, "z", [(i, size - 1 - i) for i in range(size)])


def attend_kernel(at_ref, q_ref, kv_ref, out_ref, vt_major, vt_minor, accum, peak_ref):
    own_z, own_y = at_ref[0], at_ref[1]
    pair, part = pl.program_id(0), pl.program_id(1)
    chunks, length = kv_ref.shape[0], kv_ref.shape[1]
    half = length // 2
    last = jnp.where(part == 0, own_z, chunks - 1 - own_z)

    @pl.when((pair == 0) & (part == 0))
    def _():
        def turn(c, _):
            vt_major[c, :128] = kv_ref[c, :, 128:256].T
            vt_major[c, 128:] = jnp.ones((16, length), jnp.bfloat16)
            vt_minor[c, :64] = kv_ref[c, :, 256:384].T[64:]
            vt_minor[c, 64:] = jnp.ones((16, length), jnp.bfloat16)
            return 0

        lax.fori_loop(0, jnp.maximum(own_z, chunks - 1 - own_z) + 1, turn, 0)

    q = q_ref[...].reshape(length, q_ref.shape[2])
    lane = lax.broadcasted_iota(jnp.int32, (length, 128), 1)
    major = q[:, :128]
    minor = jnp.concatenate([q[:, 128:192], jnp.zeros((length, 64), q.dtype)], axis=1)
    zero = jnp.zeros_like(major)
    maps = (
        jnp.where(lane < 64, major, zero),
        jnp.where(lane >= 64, major, zero),
        jnp.where(lane < 32, minor, zero),
        jnp.where(lane >= 32, minor, zero),
    )
    accum[...] = jnp.zeros_like(accum)

    def fold(c, peaks, queries, columns, visible=None):
        scores = [dot(kv_ref[c, :, :128] if m < 2 else kv_ref[c, :, 256:384], queries[m], NT) for m in range(4)]
        weights, factors, new = [], [], []
        for m in range(4):
            score = scores[m] if visible is None else jnp.where(visible, scores[m], NEGATIVE)
            peak = jnp.maximum(peaks[m], jnp.max(score, axis=0, keepdims=True))
            factors.append(jnp.exp2((peaks[m] - peak) * SCALES[m]))
            weights.append(jnp.exp2((score - peak) * SCALES[m]).astype(jnp.bfloat16))
            new.append(peak)
        for m in range(4):
            values = vt_major[c] if m < 2 else vt_minor[c]
            rows = values.shape[0]
            accum[m, :rows, columns] = accum[m, :rows, columns] * factors[m] + dot(values, weights[m])
        return tuple(new)

    start = tuple(jnp.full((1, length), NEGATIVE, jnp.float32) for _ in range(4))
    peaks = lax.fori_loop(0, last, lambda c, p: fold(c, p, maps, slice(None)), start)
    peak_ref[...] = jnp.concatenate(list(peaks), axis=0)

    for side in range(2):
        block_y = pair * 2 + side

        @pl.when(own_y <= block_y)
        def _(side=side, block_y=block_y):
            columns = slice(side * half, (side + 1) * half)
            key_at = own_y * length + lax.broadcasted_iota(jnp.int32, (length, 1), 0)
            query_at = block_y * length + part * half + lax.broadcasted_iota(jnp.int32, (1, half), 1)
            visible = key_at // SEGMENT <= query_at // SEGMENT
            old = tuple(peak_ref[m : m + 1, columns] for m in range(4))
            new = fold(last, old, [q_map[columns] for q_map in maps], columns, visible)
            peak_ref[:, columns] = jnp.concatenate(list(new), axis=0)

        columns = slice(side * half, (side + 1) * half)
        out_ref[side, 0:128] = accum[0, :128, columns].astype(jnp.bfloat16)
        out_ref[side, 128:256] = accum[1, :128, columns].astype(jnp.bfloat16)
        out_ref[side, 256:320] = accum[2, :64, columns].astype(jnp.bfloat16)
        out_ref[side, 320:384] = accum[3, :64, columns].astype(jnp.bfloat16)
        totals = [accum[0, 128:129, columns], accum[1, 128:129, columns], accum[2, 64:65, columns], accum[3, 64:65, columns]]
        stats = jnp.concatenate([peak_ref[:, columns]] + totals, axis=0)
        high = stats.astype(jnp.bfloat16).astype(jnp.float32)
        middle = (stats - high).astype(jnp.bfloat16).astype(jnp.float32)
        low = stats - high - middle
        parts = jnp.concatenate([high, middle, low, jnp.zeros_like(low)], axis=0)
        out_ref[side, STATS:] = parts.astype(jnp.bfloat16)


def attend(at, q, kv):
    blocks, length, width = q.shape
    chunks = kv.shape[0]
    return pl.pallas_call(
        attend_kernel,
        grid_spec=pltpu.PrefetchScalarGridSpec(
            num_scalar_prefetch=1,
            grid=(blocks // 2, 2),
            in_specs=[
                pl.BlockSpec((2, length // 2, width), lambda i, j, at: (i, j, 0)),
                pl.BlockSpec(kv.shape, lambda i, j, at: (0, 0, 0)),
            ],
            out_specs=pl.BlockSpec((2, ROWS, length // 2), lambda i, j, at: (i, 0, j)),
            scratch_shapes=[
                pltpu.VMEM((chunks, 144, length), jnp.bfloat16),
                pltpu.VMEM((chunks, 80, length), jnp.bfloat16),
                pltpu.VMEM((4, 144, length), jnp.float32),
                pltpu.VMEM((4, length), jnp.float32),
            ],
        ),
        out_shape=jax.ShapeDtypeStruct((blocks, ROWS, length), jnp.bfloat16),
        compiler_params=pltpu.CompilerParams(vmem_limit_bytes=48 * 2**20),
        cost_estimate=pl.CostEstimate(flops=10**10, transcendentals=2 * 10**7, bytes_accessed=6 * 10**6),
        name="attend",
    )(at, q, kv)


def merge_kernel(lam_ref, gain_major, gain_minor, part_ref, early_ref, late_ref):
    pieces = part_ref.shape[0]
    stats = []
    for p in range(pieces):
        coded = part_ref[p, STATS:].astype(jnp.float32)
        stats.append(coded[0:8] + coded[8:16] + coded[16:24])
    row = lax.broadcasted_iota(jnp.int32, (4, stats[0].shape[1]), 0)
    scale = jnp.where(row < 2, SCALES[0], SCALES[2])
    peak = stats[0][:4]
    for p in range(1, pieces):
        peak = jnp.maximum(peak, stats[p][:4])
    factors = [jnp.exp2((s[:4] - peak) * scale) for s in stats]
    total = factors[0] * stats[0][4:]
    for p in range(1, pieces):
        total = total + factors[p] * stats[p][4:]
    factors = [f / total for f in factors]

    def head(first, size, m, lam, gain):
        def summed(at, which):
            out = factors[0][which : which + 1] * part_ref[0, at : at + size].astype(jnp.float32)
            for p in range(1, pieces):
                out = out + factors[p][which : which + 1] * part_ref[p, at : at + size].astype(jnp.float32)
            return out

        diff = summed(first, m) - lam * summed(first + size, m + 1)
        mean = jnp.mean(diff * diff, axis=0, keepdims=True)
        return diff * lax.rsqrt(mean + EPSILON) * gain

    major = head(0, 128, 0, lam_ref[0], gain_major[...])
    minor = head(256, 64, 2, lam_ref[1], gain_minor[...])
    half = major.shape[1] // 2
    for first, ref in ((0, early_ref), (half, late_ref)):
        ref[:half] = major[:, first : first + half].T.astype(jnp.bfloat16)
        turned = minor[:, first : first + half].T
        ref[half:] = jnp.concatenate([turned[: half // 2], turned[half // 2 :]], axis=1).astype(jnp.bfloat16)


def merge(lams, gain_major, gain_minor, parts):
    length = parts.shape[2]
    whole = pl.BlockSpec(memory_space=pltpu.VMEM)
    return pl.pallas_call(
        merge_kernel,
        in_specs=[pl.BlockSpec(memory_space=pltpu.SMEM), whole, whole, whole],
        out_specs=[whole, whole],
        out_shape=[jax.ShapeDtypeStruct((length * 3 // 4, 128), jnp.bfloat16)] * 2,
        name="merge",
    )(lams, gain_major, gain_minor, parts)


def mix_kernel(at_ref, heads0, heads1, gain_ref, *refs):
    fixed, (stream_ref, normed_ref, w, residual, x, stream, sems) = refs[:8], refs[8:]
    own_x, own_c = at_ref[0], at_ref[1]
    copies = []
    for i in range(8):
        side, d = divmod(i, 4)
        token = ((own_x - d) % 4 * 2 + (own_c + side) % 2) * 64
        piece = fixed[i]
        pairs = (
            (piece.at[pl.ds(0, 128)], w.at[pl.ds(i * 128, 128)]),
            (piece.at[pl.ds(128, 64)], w.at[pl.ds(1024 + i * 64, 64)]),
            (piece.at[pl.ds(192, 64)], residual.at[pl.ds(pl.multiple_of(token, 64), 64)]),
        )
        for k, (source, target) in enumerate(pairs):
            copies.append(pltpu.make_async_copy(source, target, sems.at[i, k]))
    for copy in copies:
        copy.start()
    for i in range(8):
        side, d = divmod(i, 4)
        heads = (heads0, heads1)[side]
        for h in range(2):
            at = h * 256
            x[at : at + 256, i * 128 : (i + 1) * 128] = heads[h * 4 + d, :256]
            columns = slice(1024 + i * 64, 1024 + (i + 1) * 64)
            x[at : at + 128, columns] = heads[h * 4 + d, 256:, :64]
            x[at + 128 : at + 256, columns] = heads[h * 4 + d, 256:, 64:]
    for copy in copies:
        copy.wait()
    for h in range(2):
        at = slice(h * 256, (h + 1) * 256)
        value = dot(x[at, :], w[...]) + residual[at, :].astype(jnp.float32)
        stream[at, :] = value
        mean = jnp.mean(value * value, axis=1, keepdims=True)
        normed_ref[at, :] = (value * lax.rsqrt(mean + EPSILON) * gain_ref[...]).astype(jnp.bfloat16)
    own = pl.ds(pl.multiple_of((own_x * 2 + own_c) * 64, 64), 64)
    stream_ref[...] = stream[own, :]


def mix(at, heads, fixed, gain):
    length, width = 512, fixed[0].shape[1]
    whole = pl.BlockSpec(memory_space=pltpu.VMEM)
    return pl.pallas_call(
        mix_kernel,
        in_specs=[pl.BlockSpec(memory_space=pltpu.SMEM)] + [whole] * 3 + [pl.BlockSpec(memory_space=pl.ANY)] * 8,
        out_specs=[whole, whole],
        out_shape=[
            jax.ShapeDtypeStruct((64, width), jnp.float32),
            jax.ShapeDtypeStruct((length, width), jnp.bfloat16),
        ],
        scratch_shapes=[
            pltpu.VMEM((1536, width), jnp.bfloat16),
            pltpu.VMEM((length, width), jnp.bfloat16),
            pltpu.VMEM((length, 1536), jnp.bfloat16),
            pltpu.VMEM((length, width), jnp.float32),
            pltpu.SemaphoreType.DMA((8, 3)),
        ],
        compiler_params=pltpu.CompilerParams(vmem_limit_bytes=40 * 2**20),
        cost_estimate=pl.CostEstimate(flops=33 * 10**8, transcendentals=0, bytes_accessed=12 * 10**6),
        name="mix",
    )(at, heads[0], heads[1], gain, *fixed)


def feed_kernel(at_ref, normed, weights, keep_ref, send_ref, up, down, hidden, sems):
    own_c = at_ref[1]
    width = up.shape[1]
    copies = [
        pltpu.make_async_copy(weights.at[:, pl.ds(k * width, width)], target, sems.at[k])
        for k, target in enumerate((up, down))
    ]
    for copy in copies:
        copy.start()
    copies[0].wait()
    for h in range(2):
        value = jnp.maximum(dot(normed[h * 256 : (h + 1) * 256, :], up[...]), 0.0)
        value = (value * value).astype(jnp.bfloat16)
        for k in range(4):
            x, c = h * 2 + k // 2, k % 2
            target = (own_c + c) % 2 * 256 + x * 64
            hidden[pl.ds(pl.multiple_of(target, 64), 64), :] = value[k * 64 : (k + 1) * 64]
    copies[1].wait()
    for side, ref in enumerate((keep_ref, send_ref)):
        out = dot(hidden[side * 256 : (side + 1) * 256, :], down[...], NT)
        ref[...] = out.astype(jnp.bfloat16).reshape(ref.shape)


def feed(at, normed, weights):
    length, width = normed.shape
    whole = pl.BlockSpec(memory_space=pltpu.VMEM)
    shape = jax.ShapeDtypeStruct((4, 64, width), jnp.bfloat16)
    inner = weights.shape[1] // 2
    return pl.pallas_call(
        feed_kernel,
        in_specs=[pl.BlockSpec(memory_space=pltpu.SMEM), whole, pl.BlockSpec(memory_space=pl.ANY)],
        out_specs=[whole, whole],
        out_shape=[shape, shape],
        scratch_shapes=[
            pltpu.VMEM((width, inner), jnp.bfloat16),
            pltpu.VMEM((width, inner), jnp.bfloat16),
            pltpu.VMEM((length, inner), jnp.bfloat16),
            pltpu.SemaphoreType.DMA((2,)),
        ],
        compiler_params=pltpu.CompilerParams(vmem_limit_bytes=40 * 2**20),
        cost_estimate=pl.CostEstimate(flops=44 * 10**8, transcendentals=0, bytes_accessed=14 * 10**6),
        name="feed",
    )(at, normed, weights)


def along_x(value):
    return [value] + [shifted(value, "x", d) for d in (1, 2, 3)]


def body(
    residual,
    query_major,
    keys_major,
    values_major,
    query_minor,
    keys_minor,
    values_minor,
    lambda_major,
    lambda_minor,
    gain_major,
    gain_minor,
    output_major,
    output_minor,
    mixer_gain,
    up_weight,
    down_weight,
):
    z, y, x, c = (lax.axis_index(a) for a in ("z", "y", "x", "c"))
    kv = jnp.concatenate([keys_major, values_major, keys_minor, values_minor], axis=1)
    kv = lax.all_gather(kv, "z")
    q = jnp.concatenate([query_major, query_minor], axis=1)
    half = q.shape[0] // 2
    q = lax.all_gather(jnp.concatenate([q[:half], mirrored(q[half:])], axis=0), "y")
    weights = jnp.concatenate([up_weight, down_weight.T], axis=1)
    weights = lax.all_gather(weights, SP, tiled=True)
    fixed = jnp.concatenate([output_major, output_minor, residual], axis=0)
    fixed, q = lax.optimization_barrier((fixed, q))
    fixed = along_x(fixed)

    parts = attend(jnp.stack([z, y]).astype(jnp.int32), q, kv)
    parts, *fixed = lax.optimization_barrier((parts, *fixed))
    fixed = fixed + [shifted(f, "c", 1) for f in fixed]
    parts = lax.all_to_all(parts, "y", 0, 0, tiled=True)
    lams = jnp.concatenate([lambda_major, lambda_minor])
    early, late = merge(lams, gain_major[:, None], gain_minor[:, None], parts)
    heads = jnp.stack(along_x(early) + along_x(mirrored(late)))
    heads = (heads, shifted(heads, "c", 1))
    at = jnp.stack([x, c]).astype(jnp.int32)
    stream, normed = mix(at, heads, fixed, mixer_gain[None])
    keep, send = feed(at, normed, weights)
    pair = keep.astype(jnp.float32) + shifted(send, "c", 1).astype(jnp.float32)
    blocks = lax.all_to_all(pair.astype(jnp.bfloat16), "x", 0, 0, tiled=True)
    return (stream + jnp.sum(blocks.astype(jnp.float32), axis=0)).astype(jnp.bfloat16)


def solution(mesh):
    finer = Mesh(mesh.devices.reshape(8, 4, 4, 2), ("z", "y", "x", "c"))
    placed = (
        P(SP + TP, None),
        P(SP, TP),
        P(SP, TP),
        P(SP, TP),
        P(SP, TP),
        P(SP, TP),
        P(SP, TP),
        P(TP),
        P(TP),
        P(),
        P(),
        P(TP, None),
        P(TP, None),
        P(),
        P(SP, TP),
        P(TP, SP),
    )
    return jax.shard_map(
        body, mesh=finer, in_specs=placed, out_specs=P(SP + TP, None), check_vma=False
    )
```

```python
import jax
import jax.numpy as jnp
from jax import lax
from jax.experimental import pallas as pl
from jax.experimental.pallas import tpu as pltpu
from jax.sharding import Mesh
from jax.sharding import PartitionSpec as P

DK_MAJOR = 64
DK_MINOR = 32
SEGMENT = 64
EPSILON = 1e-06
NEGATIVE = -1e30
LOG2E = 1.4426950408889634
SCALES = (DK_MAJOR**-0.5 * LOG2E,) * 2 + (DK_MINOR**-0.5 * LOG2E,) * 2
SP = ("z", "y")
TP = ("x", "c")
ROWS = 416
STATS = 384
NT = (((1,), (1,)), ((), ()))


def dot(a, b, dims=(((1,), (0,)), ((), ()))):
    return lax.dot_general(a, b, dims, preferred_element_type=jnp.float32)


def shifted(value, axis, by):
    size = lax.axis_size(axis)
    return lax.ppermute(value, axis, [(i, (i + by) % size) for i in range(size)])


def mirrored(value):
    size = lax.axis_size("z")
    return lax.ppermute(value, "z", [(i, size - 1 - i) for i in range(size)])


def attend_kernel(at_ref, q_ref, kv_ref, out_ref, vt_major, vt_minor, k_minor, accum, peak_ref):
    own_y, part, last = at_ref[0], at_ref[1], at_ref[2]
    pair = pl.program_id(0)
    length = vt_major.shape[2]
    half = length // 2

    @pl.when(pair == 0)
    def _():
        def turn(c, _):
            vt_major[c, :128] = kv_ref[c, :length, 128:256].T
            vt_major[c, 128:] = jnp.ones((16, length), jnp.bfloat16)
            for h in range(2):
                minor = kv_ref[c, length + h * 128 : length + (h + 1) * 128]
                vt_minor[c, :64, h * half : (h + 1) * half] = minor[64:]
                k_minor[c, h * half : (h + 1) * half] = minor.T
            vt_minor[c, 64:] = jnp.ones((16, length), jnp.bfloat16)
            return 0

        lax.fori_loop(0, last + 1, turn, 0)

    q = q_ref[...].reshape(length, q_ref.shape[2])
    lane = lax.broadcasted_iota(jnp.int32, (length, 128), 1)
    major = q[:, :128]
    minor = jnp.concatenate([q[:, 128:192], jnp.zeros((length, 64), q.dtype)], axis=1)
    zero = jnp.zeros_like(major)
    maps = (
        jnp.where(lane < 64, major, zero),
        jnp.where(lane >= 64, major, zero),
        jnp.where(lane < 32, minor, zero),
        jnp.where(lane >= 32, minor, zero),
    )
    accum[...] = jnp.zeros_like(accum)

    def fold(c, peaks, queries, columns, visible=None):
        scores = [dot(kv_ref[c, :length, :128] if m < 2 else k_minor[c], queries[m], NT) for m in range(4)]
        weights, factors, new = [], [], []
        for m in range(4):
            score = scores[m] if visible is None else jnp.where(visible, scores[m], NEGATIVE)
            peak = jnp.maximum(peaks[m], jnp.max(score, axis=0, keepdims=True))
            factors.append(jnp.exp2((peaks[m] - peak) * SCALES[m]))
            weights.append(jnp.exp2((score - peak) * SCALES[m]).astype(jnp.bfloat16))
            new.append(peak)
        for m in range(4):
            values = vt_major[c] if m < 2 else vt_minor[c]
            rows = values.shape[0]
            accum[m, :rows, columns] = accum[m, :rows, columns] * factors[m] + dot(values, weights[m])
        return tuple(new)

    start = tuple(jnp.full((1, length), NEGATIVE, jnp.float32) for _ in range(4))
    peaks = lax.fori_loop(0, last, lambda c, p: fold(c, p, maps, slice(None)), start)
    peak_ref[...] = jnp.concatenate(list(peaks), axis=0)

    for side in range(2):
        block_y = pair * 2 + side

        @pl.when(own_y <= block_y)
        def _(side=side, block_y=block_y):
            columns = slice(side * half, (side + 1) * half)
            key_at = own_y * length + lax.broadcasted_iota(jnp.int32, (length, 1), 0)
            query_at = block_y * length + part * half + lax.broadcasted_iota(jnp.int32, (1, half), 1)
            visible = key_at // SEGMENT <= query_at // SEGMENT
            old = tuple(peak_ref[m : m + 1, columns] for m in range(4))
            new = fold(last, old, [q_map[columns] for q_map in maps], columns, visible)
            peak_ref[:, columns] = jnp.concatenate(list(new), axis=0)

        columns = slice(side * half, (side + 1) * half)
        out_ref[side, 0:128] = accum[0, :128, columns].astype(jnp.bfloat16)
        out_ref[side, 128:256] = accum[1, :128, columns].astype(jnp.bfloat16)
        out_ref[side, 256:320] = accum[2, :64, columns].astype(jnp.bfloat16)
        out_ref[side, 320:384] = accum[3, :64, columns].astype(jnp.bfloat16)
        totals = [accum[0, 128:129, columns], accum[1, 128:129, columns], accum[2, 64:65, columns], accum[3, 64:65, columns]]
        stats = jnp.concatenate([peak_ref[:, columns]] + totals, axis=0)
        high = stats.astype(jnp.bfloat16).astype(jnp.float32)
        middle = (stats - high).astype(jnp.bfloat16).astype(jnp.float32)
        low = stats - high - middle
        parts = jnp.concatenate([high, middle, low, jnp.zeros_like(low)], axis=0)
        out_ref[side, STATS:] = parts.astype(jnp.bfloat16)


def attend(at, q, kv):
    blocks, length, width = q.shape
    chunks = kv.shape[0]
    return pl.pallas_call(
        attend_kernel,
        grid_spec=pltpu.PrefetchScalarGridSpec(
            num_scalar_prefetch=1,
            grid=(blocks // 2,),
            in_specs=[
                pl.BlockSpec((2, length // 2, width), lambda i, at: (i, at[1], 0)),
                pl.BlockSpec(kv.shape, lambda i, at: (0, 0, 0)),
            ],
            out_specs=pl.BlockSpec((2, ROWS, length // 2), lambda i, at: (i, 0, 0)),
            scratch_shapes=[
                pltpu.VMEM((chunks, 144, length), jnp.bfloat16),
                pltpu.VMEM((chunks, 80, length), jnp.bfloat16),
                pltpu.VMEM((chunks, length, 128), jnp.bfloat16),
                pltpu.VMEM((4, 144, length), jnp.float32),
                pltpu.VMEM((4, length), jnp.float32),
            ],
        ),
        out_shape=jax.ShapeDtypeStruct((blocks, ROWS, length // 2), jnp.bfloat16),
        compiler_params=pltpu.CompilerParams(vmem_limit_bytes=60 * 2**20),
        cost_estimate=pl.CostEstimate(flops=10**10, transcendentals=2 * 10**7, bytes_accessed=6 * 10**6),
    )(at, q, kv)


def merged(lam_ref, gain_major, gain_minor, part_ref):
    pieces = part_ref.shape[0]
    stats = []
    for p in range(pieces):
        coded = part_ref[p, STATS:].astype(jnp.float32)
        stats.append(coded[0:8] + coded[8:16] + coded[16:24])
    row = lax.broadcasted_iota(jnp.int32, (4, stats[0].shape[1]), 0)
    scale = jnp.where(row < 2, SCALES[0], SCALES[2])
    peak = stats[0][:4]
    for p in range(1, pieces):
        peak = jnp.maximum(peak, stats[p][:4])
    factors = [jnp.exp2((s[:4] - peak) * scale) for s in stats]
    total = factors[0] * stats[0][4:]
    for p in range(1, pieces):
        total = total + factors[p] * stats[p][4:]
    factors = [f / total for f in factors]

    def head(first, size, m, lam, gain):
        def summed(at, which):
            out = factors[0][which : which + 1] * part_ref[0, at : at + size].astype(jnp.float32)
            for p in range(1, pieces):
                out = out + factors[p][which : which + 1] * part_ref[p, at : at + size].astype(jnp.float32)
            return out

        diff = summed(first, m) - lam * summed(first + size, m + 1)
        mean = jnp.mean(diff * diff, axis=0, keepdims=True)
        return (diff * lax.rsqrt(mean + EPSILON) * gain).T

    major = head(0, 128, 0, lam_ref[0], gain_major[...])
    minor = head(256, 64, 2, lam_ref[1], gain_minor[...])
    rows = minor.shape[0] // 2
    minor = jnp.concatenate([minor[:rows], minor[rows:]], axis=1)
    return jnp.concatenate([major, minor], axis=0)


def merge_kernel(first_ref, lam_ref, gain_major, gain_minor, short_ref, long_ref, early_ref, late_ref):
    short = merged(lam_ref, gain_major, gain_minor, short_ref)
    long = merged(lam_ref, gain_major, gain_minor, long_ref)
    swap = first_ref[0] == 1
    early_ref[...] = jnp.where(swap, long, short).astype(jnp.bfloat16)
    late_ref[...] = jnp.where(swap, short, long).astype(jnp.bfloat16)


def merge(first, lams, gain_major, gain_minor, short, long):
    half = short.shape[2]
    whole = pl.BlockSpec(memory_space=pltpu.VMEM)
    scalars = pl.BlockSpec(memory_space=pltpu.SMEM)
    return pl.pallas_call(
        merge_kernel,
        in_specs=[scalars, scalars] + [whole] * 4,
        out_specs=[whole, whole],
        out_shape=[jax.ShapeDtypeStruct((half * 3 // 2, 128), jnp.bfloat16)] * 2,
        name="merge",
    )(first, lams, gain_major, gain_minor, short, long)


def mix_kernel(at_ref, heads0, heads1, gain_ref, *refs):
    fixed, (stream_ref, normed_ref, w, residual, x, stream, sems) = refs[:8], refs[8:]
    own_x, own_c = at_ref[0], at_ref[1]
    copies = []
    for i in range(8):
        side, d = divmod(i, 4)
        place = (own_x - d) % 4
        token = (place * 2 + (own_c + side) % 2) * 64
        piece = fixed[i]
        pairs = (
            (piece.at[pl.ds(0, 128)], w.at[pl.ds(i * 128, 128)]),
            (piece.at[pl.ds(128, 64)], w.at[pl.ds(1024 + i * 64, 64)]),
            (piece.at[pl.ds(192, 64)], residual.at[pl.ds(pl.multiple_of(token, 64), 64)]),
        )
        for k, (source, target) in enumerate(pairs):
            copies.append(pltpu.make_async_copy(source, target, sems.at[i, k]))
    for copy in copies:
        copy.start()
    for i in range(8):
        side, d = divmod(i, 4)
        heads = (heads0, heads1)[side]
        for h in range(2):
            at = h * 256
            x[at : at + 256, i * 128 : (i + 1) * 128] = heads[h * 4 + d, :256]
            columns = slice(1024 + i * 64, 1024 + (i + 1) * 64)
            x[at : at + 128, columns] = heads[h * 4 + d, 256:, :64]
            x[at + 128 : at + 256, columns] = heads[h * 4 + d, 256:, 64:]
    for copy in copies:
        copy.wait()
    for h in range(2):
        at = slice(h * 256, (h + 1) * 256)
        value = dot(x[at, :], w[...]) + residual[at, :].astype(jnp.float32)
        stream[at, :] = value
        mean = jnp.mean(value * value, axis=1, keepdims=True)
        normed_ref[at, :] = (value * lax.rsqrt(mean + EPSILON) * gain_ref[...]).astype(jnp.bfloat16)
    own = pl.ds(pl.multiple_of((own_x * 2 + own_c) * 64, 64), 64)
    stream_ref[...] = stream[own, :]


def mix(at, heads, fixed, gain):
    length, width = 512, fixed[0].shape[1]
    whole = pl.BlockSpec(memory_space=pltpu.VMEM)
    return pl.pallas_call(
        mix_kernel,
        in_specs=[pl.BlockSpec(memory_space=pltpu.SMEM)] + [whole] * 3 + [pl.BlockSpec(memory_space=pl.ANY)] * 8,
        out_specs=[whole, whole],
        out_shape=[
            jax.ShapeDtypeStruct((64, width), jnp.float32),
            jax.ShapeDtypeStruct((length, width), jnp.bfloat16),
        ],
        scratch_shapes=[
            pltpu.VMEM((1536, width), jnp.bfloat16),
            pltpu.VMEM((length, width), jnp.bfloat16),
            pltpu.VMEM((length, 1536), jnp.bfloat16),
            pltpu.VMEM((length, width), jnp.float32),
            pltpu.SemaphoreType.DMA((8, 3)),
        ],
        compiler_params=pltpu.CompilerParams(vmem_limit_bytes=60 * 2**20),
        cost_estimate=pl.CostEstimate(flops=33 * 10**8, transcendentals=0, bytes_accessed=12 * 10**6),
        name="mix",
    )(at, heads[0], heads[1], gain, *fixed)


def feed_kernel(at_ref, normed, weights, keep_ref, send_ref, up, down, hidden, sems):
    own_c, own_y = at_ref[1], at_ref[2]
    rows, width = normed.shape[1], up.shape[3]
    copies = [
        [
            pltpu.make_async_copy(
                weights.at[:, d, :, pl.ds(k * width, width)], target.at[:, (own_y - d) % 4], sems.at[k, d]
            )
            for d in range(4)
        ]
        for k, target in enumerate((up, down))
    ]
    for copy in copies[0] + copies[1]:
        copy.start()
    for copy in copies[0]:
        copy.wait()
    for h in range(2):
        value = jnp.maximum(dot(normed[h * 256 : (h + 1) * 256, :], up[...].reshape(rows, width)), 0.0)
        value = (value * value).astype(jnp.bfloat16)
        for k in range(4):
            x, c = h * 2 + k // 2, k % 2
            target = (own_c + c) % 2 * 256 + x * 64
            hidden[pl.ds(pl.multiple_of(target, 64), 64), :] = value[k * 64 : (k + 1) * 64]
    for copy in copies[1]:
        copy.wait()
    for side, ref in enumerate((keep_ref, send_ref)):
        out = dot(hidden[side * 256 : (side + 1) * 256, :], down[...].reshape(rows, width), NT)
        ref[...] = out.astype(jnp.bfloat16).reshape(ref.shape)


def feed(at, normed, weights):
    length, width = normed.shape
    whole = pl.BlockSpec(memory_space=pltpu.VMEM)
    shape = jax.ShapeDtypeStruct((4, 64, width), jnp.bfloat16)
    inner = weights.shape[3] // 2
    gathered = pltpu.VMEM(weights.shape[:3] + (inner,), jnp.bfloat16)
    return pl.pallas_call(
        feed_kernel,
        in_specs=[pl.BlockSpec(memory_space=pltpu.SMEM), whole, pl.BlockSpec(memory_space=pltpu.HBM)],
        out_specs=[whole, whole],
        out_shape=[shape, shape],
        scratch_shapes=[
            gathered,
            gathered,
            pltpu.VMEM((length, inner), jnp.bfloat16),
            pltpu.SemaphoreType.DMA((2, 4)),
        ],
        compiler_params=pltpu.CompilerParams(vmem_limit_bytes=60 * 2**20),
        cost_estimate=pl.CostEstimate(flops=44 * 10**8, transcendentals=0, bytes_accessed=14 * 10**6),
        name="feed",
    )(at, normed, weights)


def along(value, axis):
    return [value] + [shifted(value, axis, d) for d in (1, 2, 3)]


def body(
    residual,
    query_major,
    keys_major,
    values_major,
    query_minor,
    keys_minor,
    values_minor,
    lambda_major,
    lambda_minor,
    gain_major,
    gain_minor,
    output_major,
    output_minor,
    mixer_gain,
    up_weight,
    down_weight,
):
    z, y, x, c = (lax.axis_index(a) for a in ("z", "y", "x", "c"))
    minor = jnp.concatenate([keys_minor.T, values_minor.T], axis=0)
    kv = jnp.concatenate([keys_major, values_major], axis=1)
    kv = jnp.concatenate([kv, minor[:, :256], minor[:, 256:]], axis=0)
    kv = lax.all_gather(kv, "z")
    q = jnp.concatenate([query_major, query_minor], axis=1)
    half = q.shape[0] // 2
    q = jnp.concatenate([q[:half], mirrored(q[half:])], axis=0)
    fixed = jnp.concatenate([output_major, output_minor, residual], axis=0)
    fixed = along(fixed, "x")
    q = lax.all_gather(q, "y")
    weights = jnp.concatenate([up_weight, down_weight.T], axis=1)
    weights, q = lax.optimization_barrier((weights, q))
    weights = lax.all_gather(jnp.stack(along(weights, "y")), "z")

    mirror = lax.axis_size("z") - 1 - z
    short_part = (z > mirror).astype(jnp.int32)
    short = attend(jnp.stack([y, short_part, jnp.minimum(z, mirror)]), q, kv)
    short = lax.all_to_all(short, "y", 0, 0, tiled=True)
    long = attend(jnp.stack([y, 1 - short_part, jnp.maximum(z, mirror)]), q, kv)
    long, *fixed = lax.optimization_barrier((long, *fixed))
    fixed = fixed + [shifted(f, "c", 1) for f in fixed]
    long = lax.all_to_all(long, "y", 0, 0, tiled=True)
    lams = jnp.concatenate([lambda_major, lambda_minor])
    early, late = merge(short_part[None], lams, gain_major[:, None], gain_minor[:, None], short, long)
    heads = jnp.stack(along(early, "x") + along(mirrored(late), "x"))
    heads = (heads, shifted(heads, "c", 1))
    at = jnp.stack([x, c, y]).astype(jnp.int32)
    stream, normed = mix(at, heads, fixed, mixer_gain[None])
    keep, send = feed(at, normed, weights)
    pair = keep.astype(jnp.float32) + shifted(send, "c", 1).astype(jnp.float32)
    blocks = lax.all_to_all(pair.astype(jnp.bfloat16), "x", 0, 0, tiled=True)
    return (stream + jnp.sum(blocks.astype(jnp.float32), axis=0)).astype(jnp.bfloat16)


def solution(mesh):
    finer = Mesh(mesh.devices.reshape(8, 4, 4, 2), ("z", "y", "x", "c"))
    placed = (
        P(SP + TP, None),
        P(SP, TP),
        P(SP, TP),
        P(SP, TP),
        P(SP, TP),
        P(SP, TP),
        P(SP, TP),
        P(TP),
        P(TP),
        P(),
        P(),
        P(TP, None),
        P(TP, None),
        P(),
        P(SP, TP),
        P(TP, SP),
    )

    return jax.shard_map(body, mesh=finer, in_specs=placed, out_specs=P(SP + TP, None), check_vma=False)
```

```python
import jax
import jax.numpy as jnp
from jax import lax
from jax.experimental import pallas as pl
from jax.experimental.pallas import tpu as pltpu
from jax.sharding import Mesh
from jax.sharding import PartitionSpec as P

DK_MAJOR = 64
DK_MINOR = 32
SEGMENT = 64
EPSILON = 1e-06
NEGATIVE = -1e30
LOG2E = 1.4426950408889634
SCALES = (DK_MAJOR**-0.5 * LOG2E,) * 2 + (DK_MINOR**-0.5 * LOG2E,) * 2
SP = ("z", "y")
TP = ("x", "c")
ROWS = 416
STATS = 384
NT = (((1,), (1,)), ((), ()))


def dot(a, b, dims=(((1,), (0,)), ((), ()))):
    return lax.dot_general(a, b, dims, preferred_element_type=jnp.float32)


def shifted(value, axis, by):
    size = lax.axis_size(axis)
    return lax.ppermute(value, axis, [(i, (i + by) % size) for i in range(size)])


def mirrored(value):
    size = lax.axis_size("z")
    return lax.ppermute(value, "z", [(i, size - 1 - i) for i in range(size)])


def attend_kernel(at_ref, q_ref, kv_ref, out_ref, vt_major, vt_minor, k_minor, accum, peak_ref):
    own_y, part, last = at_ref[0], at_ref[1], at_ref[2]
    pair = pl.program_id(0)
    length = vt_major.shape[2]
    half = length // 2

    @pl.when(pair == 0)
    def _():
        def turn(c, _):
            vt_major[c, :128] = kv_ref[c, :length, 128:256].T
            vt_major[c, 128:] = jnp.ones((16, length), jnp.bfloat16)
            for h in range(2):
                minor = kv_ref[c, length + h * 128 : length + (h + 1) * 128]
                vt_minor[c, :64, h * half : (h + 1) * half] = minor[64:]
                k_minor[c, h * half : (h + 1) * half] = minor.T
            vt_minor[c, 64:] = jnp.ones((16, length), jnp.bfloat16)
            return 0

        lax.fori_loop(0, last + 1, turn, 0)

    q = q_ref[...].reshape(length, q_ref.shape[2])
    lane = lax.broadcasted_iota(jnp.int32, (length, 128), 1)
    major = q[:, :128]
    minor = jnp.concatenate([q[:, 128:192], jnp.zeros((length, 64), q.dtype)], axis=1)
    zero = jnp.zeros_like(major)
    maps = (
        jnp.where(lane < 64, major, zero),
        jnp.where(lane >= 64, major, zero),
        jnp.where(lane < 32, minor, zero),
        jnp.where(lane >= 32, minor, zero),
    )
    accum[...] = jnp.zeros_like(accum)

    def fold(c, peaks, queries, columns, visible=None):
        scores = [dot(kv_ref[c, :length, :128] if m < 2 else k_minor[c], queries[m], NT) for m in range(4)]
        weights, factors, new = [], [], []
        for m in range(4):
            score = scores[m] if visible is None else jnp.where(visible, scores[m], NEGATIVE)
            peak = jnp.maximum(peaks[m], jnp.max(score, axis=0, keepdims=True))
            factors.append(jnp.exp2((peaks[m] - peak) * SCALES[m]))
            weights.append(jnp.exp2((score - peak) * SCALES[m]).astype(jnp.bfloat16))
            new.append(peak)
        for m in range(4):
            values = vt_major[c] if m < 2 else vt_minor[c]
            rows = values.shape[0]
            accum[m, :rows, columns] = accum[m, :rows, columns] * factors[m] + dot(values, weights[m])
        return tuple(new)

    start = tuple(jnp.full((1, length), NEGATIVE, jnp.float32) for _ in range(4))
    peaks = lax.fori_loop(0, last, lambda c, p: fold(c, p, maps, slice(None)), start)
    peak_ref[...] = jnp.concatenate(list(peaks), axis=0)

    for side in range(2):
        block_y = pair * 2 + side

        @pl.when(own_y <= block_y)
        def _(side=side, block_y=block_y):
            columns = slice(side * half, (side + 1) * half)
            key_at = own_y * length + lax.broadcasted_iota(jnp.int32, (length, 1), 0)
            query_at = block_y * length + part * half + lax.broadcasted_iota(jnp.int32, (1, half), 1)
            visible = key_at // SEGMENT <= query_at // SEGMENT
            old = tuple(peak_ref[m : m + 1, columns] for m in range(4))
            new = fold(last, old, [q_map[columns] for q_map in maps], columns, visible)
            peak_ref[:, columns] = jnp.concatenate(list(new), axis=0)

        columns = slice(side * half, (side + 1) * half)
        out_ref[side, 0:128] = accum[0, :128, columns].astype(jnp.bfloat16)
        out_ref[side, 128:256] = accum[1, :128, columns].astype(jnp.bfloat16)
        out_ref[side, 256:320] = accum[2, :64, columns].astype(jnp.bfloat16)
        out_ref[side, 320:384] = accum[3, :64, columns].astype(jnp.bfloat16)
        totals = [accum[0, 128:129, columns], accum[1, 128:129, columns], accum[2, 64:65, columns], accum[3, 64:65, columns]]
        stats = jnp.concatenate([peak_ref[:, columns]] + totals, axis=0)
        high = stats.astype(jnp.bfloat16).astype(jnp.float32)
        middle = (stats - high).astype(jnp.bfloat16).astype(jnp.float32)
        low = stats - high - middle
        parts = jnp.concatenate([high, middle, low, jnp.zeros_like(low)], axis=0)
        out_ref[side, STATS:] = parts.astype(jnp.bfloat16)


def attend(at, q, kv):
    blocks, length, width = q.shape
    chunks = kv.shape[0]
    return pl.pallas_call(
        attend_kernel,
        grid_spec=pltpu.PrefetchScalarGridSpec(
            num_scalar_prefetch=1,
            grid=(blocks // 2,),
            in_specs=[
                pl.BlockSpec((2, length // 2, width), lambda i, at: (i, at[1], 0)),
                pl.BlockSpec(kv.shape, lambda i, at: (0, 0, 0)),
            ],
            out_specs=pl.BlockSpec((2, ROWS, length // 2), lambda i, at: (i, 0, 0)),
            scratch_shapes=[
                pltpu.VMEM((chunks, 144, length), jnp.bfloat16),
                pltpu.VMEM((chunks, 80, length), jnp.bfloat16),
                pltpu.VMEM((chunks, length, 128), jnp.bfloat16),
                pltpu.VMEM((4, 144, length), jnp.float32),
                pltpu.VMEM((4, length), jnp.float32),
            ],
        ),
        out_shape=jax.ShapeDtypeStruct((blocks, ROWS, length // 2), jnp.bfloat16),
        compiler_params=pltpu.CompilerParams(vmem_limit_bytes=60 * 2**20),
        cost_estimate=pl.CostEstimate(flops=10**10, transcendentals=2 * 10**7, bytes_accessed=6 * 10**6),
    )(at, q, kv)


def merged(lam_ref, gain_major, gain_minor, part_ref):
    pieces = part_ref.shape[0]
    stats = []
    for p in range(pieces):
        coded = part_ref[p, STATS:].astype(jnp.float32)
        stats.append(coded[0:8] + coded[8:16] + coded[16:24])
    row = lax.broadcasted_iota(jnp.int32, (4, stats[0].shape[1]), 0)
    scale = jnp.where(row < 2, SCALES[0], SCALES[2])
    peak = stats[0][:4]
    for p in range(1, pieces):
        peak = jnp.maximum(peak, stats[p][:4])
    factors = [jnp.exp2((s[:4] - peak) * scale) for s in stats]
    total = factors[0] * stats[0][4:]
    for p in range(1, pieces):
        total = total + factors[p] * stats[p][4:]
    factors = [f / total for f in factors]

    def head(first, size, m, lam, gain):
        def summed(at, which):
            out = factors[0][which : which + 1] * part_ref[0, at : at + size].astype(jnp.float32)
            for p in range(1, pieces):
                out = out + factors[p][which : which + 1] * part_ref[p, at : at + size].astype(jnp.float32)
            return out

        diff = summed(first, m) - lam * summed(first + size, m + 1)
        mean = jnp.mean(diff * diff, axis=0, keepdims=True)
        return (diff * lax.rsqrt(mean + EPSILON) * gain).T

    major = head(0, 128, 0, lam_ref[0], gain_major[...])
    minor = head(256, 64, 2, lam_ref[1], gain_minor[...])
    rows = minor.shape[0] // 2
    minor = jnp.concatenate([minor[:rows], minor[rows:]], axis=1)
    return jnp.concatenate([major, minor], axis=0)


def merge_kernel(first_ref, lam_ref, gain_major, gain_minor, short_ref, long_ref, early_ref, late_ref):
    short = merged(lam_ref, gain_major, gain_minor, short_ref)
    long = merged(lam_ref, gain_major, gain_minor, long_ref)
    swap = first_ref[0] == 1
    early_ref[...] = jnp.where(swap, long, short).astype(jnp.bfloat16)
    late_ref[...] = jnp.where(swap, short, long).astype(jnp.bfloat16)


def merge(first, lams, gain_major, gain_minor, short, long):
    half = short.shape[2]
    whole = pl.BlockSpec(memory_space=pltpu.VMEM)
    scalars = pl.BlockSpec(memory_space=pltpu.SMEM)
    return pl.pallas_call(
        merge_kernel,
        in_specs=[scalars, scalars] + [whole] * 4,
        out_specs=[whole, whole],
        out_shape=[jax.ShapeDtypeStruct((half * 3 // 2, 128), jnp.bfloat16)] * 2,
        name="merge",
    )(first, lams, gain_major, gain_minor, short, long)


def mix_kernel(at_ref, heads0, heads1, gain_ref, *refs):
    fixed, (stream_ref, normed_ref, w, residual, x, stream, sems) = refs[:8], refs[8:]
    own_x, own_c = at_ref[0], at_ref[1]
    copies = []
    for i in range(8):
        side, d = divmod(i, 4)
        place = (own_x - d) % 4
        token = (place * 2 + (own_c + side) % 2) * 64
        piece = fixed[i]
        pairs = (
            (piece.at[pl.ds(0, 128)], w.at[pl.ds(i * 128, 128)]),
            (piece.at[pl.ds(128, 64)], w.at[pl.ds(1024 + i * 64, 64)]),
            (piece.at[pl.ds(192, 64)], residual.at[pl.ds(pl.multiple_of(token, 64), 64)]),
        )
        for k, (source, target) in enumerate(pairs):
            copies.append(pltpu.make_async_copy(source, target, sems.at[i, k]))
    for copy in copies:
        copy.start()
    for i in range(8):
        side, d = divmod(i, 4)
        heads = (heads0, heads1)[side]
        for h in range(2):
            at = h * 256
            x[at : at + 256, i * 128 : (i + 1) * 128] = heads[h * 4 + d, :256]
            columns = slice(1024 + i * 64, 1024 + (i + 1) * 64)
            x[at : at + 128, columns] = heads[h * 4 + d, 256:, :64]
            x[at + 128 : at + 256, columns] = heads[h * 4 + d, 256:, 64:]
    for copy in copies:
        copy.wait()
    for h in range(2):
        at = slice(h * 256, (h + 1) * 256)
        value = dot(x[at, :], w[...]) + residual[at, :].astype(jnp.float32)
        stream[at, :] = value
        mean = jnp.mean(value * value, axis=1, keepdims=True)
        normed_ref[at, :] = (value * lax.rsqrt(mean + EPSILON) * gain_ref[...]).astype(jnp.bfloat16)
    own = pl.ds(pl.multiple_of((own_x * 2 + own_c) * 64, 64), 64)
    stream_ref[...] = stream[own, :]


def mix(at, heads, fixed, gain):
    length, width = 512, fixed[0].shape[1]
    whole = pl.BlockSpec(memory_space=pltpu.VMEM)
    return pl.pallas_call(
        mix_kernel,
        in_specs=[pl.BlockSpec(memory_space=pltpu.SMEM)] + [whole] * 3 + [pl.BlockSpec(memory_space=pl.ANY)] * 8,
        out_specs=[whole, whole],
        out_shape=[
            jax.ShapeDtypeStruct((64, width), jnp.float32),
            jax.ShapeDtypeStruct((length, width), jnp.bfloat16),
        ],
        scratch_shapes=[
            pltpu.VMEM((1536, width), jnp.bfloat16),
            pltpu.VMEM((length, width), jnp.bfloat16),
            pltpu.VMEM((length, 1536), jnp.bfloat16),
            pltpu.VMEM((length, width), jnp.float32),
            pltpu.SemaphoreType.DMA((8, 3)),
        ],
        compiler_params=pltpu.CompilerParams(vmem_limit_bytes=60 * 2**20),
        cost_estimate=pl.CostEstimate(flops=33 * 10**8, transcendentals=0, bytes_accessed=12 * 10**6),
        name="mix",
    )(at, heads[0], heads[1], gain, *fixed)


def feed_kernel(at_ref, normed, weights, keep_ref, send_ref, up, down, hidden, sems):
    own_c, own_y = at_ref[1], at_ref[2]
    rows, width = normed.shape[1], up.shape[3]
    copies = [
        [
            pltpu.make_async_copy(
                weights.at[:, d, :, pl.ds(k * width, width)], target.at[:, (own_y - d) % 4], sems.at[k, d]
            )
            for d in range(4)
        ]
        for k, target in enumerate((up, down))
    ]
    for copy in copies[0] + copies[1]:
        copy.start()
    for copy in copies[0]:
        copy.wait()
    for h in range(2):
        value = jnp.maximum(dot(normed[h * 256 : (h + 1) * 256, :], up[...].reshape(rows, width)), 0.0)
        value = (value * value).astype(jnp.bfloat16)
        for k in range(4):
            x, c = h * 2 + k // 2, k % 2
            target = (own_c + c) % 2 * 256 + x * 64
            hidden[pl.ds(pl.multiple_of(target, 64), 64), :] = value[k * 64 : (k + 1) * 64]
    for copy in copies[1]:
        copy.wait()
    for side, ref in enumerate((keep_ref, send_ref)):
        out = dot(hidden[side * 256 : (side + 1) * 256, :], down[...].reshape(rows, width), NT)
        ref[...] = out.astype(jnp.bfloat16).reshape(ref.shape)


def feed(at, normed, weights):
    length, width = normed.shape
    whole = pl.BlockSpec(memory_space=pltpu.VMEM)
    shape = jax.ShapeDtypeStruct((4, 64, width), jnp.bfloat16)
    inner = weights.shape[3] // 2
    gathered = pltpu.VMEM(weights.shape[:3] + (inner,), jnp.bfloat16)
    return pl.pallas_call(
        feed_kernel,
        in_specs=[pl.BlockSpec(memory_space=pltpu.SMEM), whole, pl.BlockSpec(memory_space=pltpu.HBM)],
        out_specs=[whole, whole],
        out_shape=[shape, shape],
        scratch_shapes=[
            gathered,
            gathered,
            pltpu.VMEM((length, inner), jnp.bfloat16),
            pltpu.SemaphoreType.DMA((2, 4)),
        ],
        compiler_params=pltpu.CompilerParams(vmem_limit_bytes=60 * 2**20),
        cost_estimate=pl.CostEstimate(flops=44 * 10**8, transcendentals=0, bytes_accessed=14 * 10**6),
        name="feed",
    )(at, normed, weights)


def along(value, axis):
    return [value] + [shifted(value, axis, d) for d in (1, 2, 3)]


def body(
    residual,
    query_major,
    keys_major,
    values_major,
    query_minor,
    keys_minor,
    values_minor,
    lambda_major,
    lambda_minor,
    gain_major,
    gain_minor,
    output_major,
    output_minor,
    mixer_gain,
    up_weight,
    down_weight,
):
    z, y, x, c = (lax.axis_index(a) for a in ("z", "y", "x", "c"))
    minor = jnp.concatenate([keys_minor.T, values_minor.T], axis=0)
    kv = jnp.concatenate([keys_major, values_major], axis=1)
    kv = jnp.concatenate([kv, minor[:, :256], minor[:, 256:]], axis=0)
    kv = lax.all_gather(kv, "z")
    q = jnp.concatenate([query_major, query_minor], axis=1)
    half = q.shape[0] // 2
    late = mirrored(q[half:])
    q = jnp.concatenate([q[:half], late], axis=0)
    fixed = jnp.concatenate([output_major, output_minor, residual], axis=0)
    fixed = along(fixed, "x")
    q = lax.all_gather(q, "y")
    weights = jnp.concatenate([up_weight, down_weight.T], axis=1)
    weights = along(weights, "y")
    weights = lax.all_gather(jnp.stack(weights), "z")

    mirror = lax.axis_size("z") - 1 - z
    short_part = (z > mirror).astype(jnp.int32)
    short = attend(jnp.stack([y, short_part, jnp.minimum(z, mirror)]), q, kv)
    short = lax.all_to_all(short, "y", 0, 0, tiled=True)
    long = attend(jnp.stack([y, 1 - short_part, jnp.maximum(z, mirror)]), q, kv)
    long, *fixed = lax.optimization_barrier((long, *fixed))
    fixed = fixed + [shifted(f, "c", 1) for f in fixed]
    long = lax.all_to_all(long, "y", 0, 0, tiled=True)
    lams = jnp.concatenate([lambda_major, lambda_minor])
    early, late = merge(short_part[None], lams, gain_major[:, None], gain_minor[:, None], short, long)
    heads = jnp.stack(along(early, "x") + along(mirrored(late), "x"))
    heads = (heads, shifted(heads, "c", 1))
    at = jnp.stack([x, c, y]).astype(jnp.int32)
    stream, normed = mix(at, heads, fixed, mixer_gain[None])
    keep, send = feed(at, normed, weights)
    pair = keep.astype(jnp.float32) + shifted(send, "c", 1).astype(jnp.float32)
    blocks = lax.all_to_all(pair.astype(jnp.bfloat16), "x", 0, 0, tiled=True)
    return (stream + jnp.sum(blocks.astype(jnp.float32), axis=0)).astype(jnp.bfloat16)


def solution(mesh):
    finer = Mesh(mesh.devices.reshape(8, 4, 4, 2), ("z", "y", "x", "c"))
    placed = (
        P(SP + TP, None),
        P(SP, TP),
        P(SP, TP),
        P(SP, TP),
        P(SP, TP),
        P(SP, TP),
        P(SP, TP),
        P(TP),
        P(TP),
        P(),
        P(),
        P(TP, None),
        P(TP, None),
        P(),
        P(SP, TP),
        P(TP, SP),
    )

    return jax.shard_map(body, mesh=finer, in_specs=placed, out_specs=P(SP + TP, None), check_vma=False)
```

```python
import jax
import jax.numpy as jnp
from jax import lax
from jax.experimental import pallas as pl
from jax.experimental.pallas import tpu as pltpu
from jax.sharding import Mesh
from jax.sharding import PartitionSpec as P

DK_MAJOR = 64
DK_MINOR = 32
SEGMENT = 64
EPSILON = 1e-06
NEGATIVE = -1e30
LOG2E = 1.4426950408889634
SCALES = (DK_MAJOR**-0.5 * LOG2E,) * 2 + (DK_MINOR**-0.5 * LOG2E,) * 2
SP = ("z", "y")
TP = ("x", "c")
ROWS = 416
STATS = 384
NT = (((1,), (1,)), ((), ()))


def dot(a, b, dims=(((1,), (0,)), ((), ()))):
    return lax.dot_general(a, b, dims, preferred_element_type=jnp.float32)


def shifted(value, axis, by):
    size = lax.axis_size(axis)
    return lax.ppermute(value, axis, [(i, (i + by) % size) for i in range(size)])


def mirrored(value):
    size = lax.axis_size("z")
    return lax.ppermute(value, "z", [(i, size - 1 - i) for i in range(size)])


def attend_kernel(at_ref, q_ref, kv_ref, out_ref, vt_major, vt_minor, k_minor, accum, peak_ref):
    own_y, part, last = at_ref[0], at_ref[1], at_ref[2]
    pair = pl.program_id(0)
    length = vt_major.shape[2]
    half = length // 2

    @pl.when(pair == 0)
    def _():
        def turn(c, _):
            vt_major[c, :128] = kv_ref[c, :length, 128:256].T
            vt_major[c, 128:] = jnp.ones((16, length), jnp.bfloat16)
            for h in range(2):
                minor = kv_ref[c, length + h * 128 : length + (h + 1) * 128]
                vt_minor[c, :64, h * half : (h + 1) * half] = minor[64:]
                k_minor[c, h * half : (h + 1) * half] = minor.T
            vt_minor[c, 64:] = jnp.ones((16, length), jnp.bfloat16)
            return 0

        lax.fori_loop(0, last + 1, turn, 0)

    q = q_ref[...].reshape(length, q_ref.shape[2])
    lane = lax.broadcasted_iota(jnp.int32, (length, 128), 1)
    major = q[:, :128]
    minor = jnp.concatenate([q[:, 128:192], jnp.zeros((length, 64), q.dtype)], axis=1)
    zero = jnp.zeros_like(major)
    maps = (
        jnp.where(lane < 64, major, zero),
        jnp.where(lane >= 64, major, zero),
        jnp.where(lane < 32, minor, zero),
        jnp.where(lane >= 32, minor, zero),
    )
    accum[...] = jnp.zeros_like(accum)

    def fold(c, peaks, queries, columns, visible=None):
        scores = [dot(kv_ref[c, :length, :128] if m < 2 else k_minor[c], queries[m], NT) for m in range(4)]
        weights, factors, new = [], [], []
        for m in range(4):
            score = scores[m] if visible is None else jnp.where(visible, scores[m], NEGATIVE)
            peak = jnp.maximum(peaks[m], jnp.max(score, axis=0, keepdims=True))
            factors.append(jnp.exp2((peaks[m] - peak) * SCALES[m]))
            weights.append(jnp.exp2((score - peak) * SCALES[m]).astype(jnp.bfloat16))
            new.append(peak)
        for m in range(4):
            values = vt_major[c] if m < 2 else vt_minor[c]
            rows = values.shape[0]
            accum[m, :rows, columns] = accum[m, :rows, columns] * factors[m] + dot(values, weights[m])
        return tuple(new)

    start = tuple(jnp.full((1, length), NEGATIVE, jnp.float32) for _ in range(4))
    peaks = lax.fori_loop(0, last, lambda c, p: fold(c, p, maps, slice(None)), start)
    peak_ref[...] = jnp.concatenate(list(peaks), axis=0)

    for side in range(2):
        block_y = pair * 2 + side

        @pl.when(own_y <= block_y)
        def _(side=side, block_y=block_y):
            columns = slice(side * half, (side + 1) * half)
            key_at = own_y * length + lax.broadcasted_iota(jnp.int32, (length, 1), 0)
            query_at = block_y * length + part * half + lax.broadcasted_iota(jnp.int32, (1, half), 1)
            visible = key_at // SEGMENT <= query_at // SEGMENT
            old = tuple(peak_ref[m : m + 1, columns] for m in range(4))
            new = fold(last, old, [q_map[columns] for q_map in maps], columns, visible)
            peak_ref[:, columns] = jnp.concatenate(list(new), axis=0)

        columns = slice(side * half, (side + 1) * half)
        out_ref[side, 0:128] = accum[0, :128, columns].astype(jnp.bfloat16)
        out_ref[side, 128:256] = accum[1, :128, columns].astype(jnp.bfloat16)
        out_ref[side, 256:320] = accum[2, :64, columns].astype(jnp.bfloat16)
        out_ref[side, 320:384] = accum[3, :64, columns].astype(jnp.bfloat16)
        totals = [accum[0, 128:129, columns], accum[1, 128:129, columns], accum[2, 64:65, columns], accum[3, 64:65, columns]]
        stats = jnp.concatenate([peak_ref[:, columns]] + totals, axis=0)
        high = stats.astype(jnp.bfloat16).astype(jnp.float32)
        middle = (stats - high).astype(jnp.bfloat16).astype(jnp.float32)
        low = stats - high - middle
        parts = jnp.concatenate([high, middle, low, jnp.zeros_like(low)], axis=0)
        out_ref[side, STATS:] = parts.astype(jnp.bfloat16)


def attend(at, q, kv):
    blocks, length, width = q.shape
    chunks = kv.shape[0]
    return pl.pallas_call(
        attend_kernel,
        grid_spec=pltpu.PrefetchScalarGridSpec(
            num_scalar_prefetch=1,
            grid=(blocks // 2,),
            in_specs=[
                pl.BlockSpec((2, length // 2, width), lambda i, at: (i, at[1], 0)),
                pl.BlockSpec(kv.shape, lambda i, at: (0, 0, 0)),
            ],
            out_specs=pl.BlockSpec((2, ROWS, length // 2), lambda i, at: (i, 0, 0)),
            scratch_shapes=[
                pltpu.VMEM((chunks, 144, length), jnp.bfloat16),
                pltpu.VMEM((chunks, 80, length), jnp.bfloat16),
                pltpu.VMEM((chunks, length, 128), jnp.bfloat16),
                pltpu.VMEM((4, 144, length), jnp.float32),
                pltpu.VMEM((4, length), jnp.float32),
            ],
        ),
        out_shape=jax.ShapeDtypeStruct((blocks, ROWS, length // 2), jnp.bfloat16),
        compiler_params=pltpu.CompilerParams(vmem_limit_bytes=60 * 2**20),
        cost_estimate=pl.CostEstimate(flops=10**10, transcendentals=2 * 10**7, bytes_accessed=6 * 10**6),
    )(at, q, kv)


def merged(lam_ref, gain_major, gain_minor, part_ref):
    pieces = part_ref.shape[0]
    stats = []
    for p in range(pieces):
        coded = part_ref[p, STATS:].astype(jnp.float32)
        stats.append(coded[0:8] + coded[8:16] + coded[16:24])
    row = lax.broadcasted_iota(jnp.int32, (4, stats[0].shape[1]), 0)
    scale = jnp.where(row < 2, SCALES[0], SCALES[2])
    peak = stats[0][:4]
    for p in range(1, pieces):
        peak = jnp.maximum(peak, stats[p][:4])
    factors = [jnp.exp2((s[:4] - peak) * scale) for s in stats]
    total = factors[0] * stats[0][4:]
    for p in range(1, pieces):
        total = total + factors[p] * stats[p][4:]
    factors = [f / total for f in factors]

    def head(first, size, m, lam, gain):
        def summed(at, which):
            out = factors[0][which : which + 1] * part_ref[0, at : at + size].astype(jnp.float32)
            for p in range(1, pieces):
                out = out + factors[p][which : which + 1] * part_ref[p, at : at + size].astype(jnp.float32)
            return out

        diff = summed(first, m) - lam * summed(first + size, m + 1)
        mean = jnp.mean(diff * diff, axis=0, keepdims=True)
        return (diff * lax.rsqrt(mean + EPSILON) * gain).T

    major = head(0, 128, 0, lam_ref[0], gain_major[...])
    minor = head(256, 64, 2, lam_ref[1], gain_minor[...])
    rows = minor.shape[0] // 2
    minor = jnp.concatenate([minor[:rows], minor[rows:]], axis=1)
    return jnp.concatenate([major, minor], axis=0)


def merge_kernel(first_ref, lam_ref, gain_major, gain_minor, short_ref, long_ref, early_ref, late_ref):
    short = merged(lam_ref, gain_major, gain_minor, short_ref)
    long = merged(lam_ref, gain_major, gain_minor, long_ref)
    swap = first_ref[0] == 1
    early_ref[...] = jnp.where(swap, long, short).astype(jnp.bfloat16)
    late_ref[...] = jnp.where(swap, short, long).astype(jnp.bfloat16)


def merge(first, lams, gain_major, gain_minor, short, long):
    half = short.shape[2]
    whole = pl.BlockSpec(memory_space=pltpu.VMEM)
    scalars = pl.BlockSpec(memory_space=pltpu.SMEM)
    return pl.pallas_call(
        merge_kernel,
        in_specs=[scalars, scalars] + [whole] * 4,
        out_specs=[whole, whole],
        out_shape=[jax.ShapeDtypeStruct((half * 3 // 2, 128), jnp.bfloat16)] * 2,
        name="merge",
    )(first, lams, gain_major, gain_minor, short, long)


def mix_kernel(at_ref, heads0, heads1, gain_ref, *refs):
    fixed, (stream_ref, normed_ref, w, residual, x, stream, sems) = refs[:8], refs[8:]
    own_x, own_c = at_ref[0], at_ref[1]
    copies = []
    for i in range(8):
        side, d = divmod(i, 4)
        place = (own_x - d) % 4
        token = (place * 2 + (own_c + side) % 2) * 64
        piece = fixed[i]
        pairs = (
            (piece.at[pl.ds(0, 128)], w.at[pl.ds(i * 128, 128)]),
            (piece.at[pl.ds(128, 64)], w.at[pl.ds(1024 + i * 64, 64)]),
            (piece.at[pl.ds(192, 64)], residual.at[pl.ds(pl.multiple_of(token, 64), 64)]),
        )
        for k, (source, target) in enumerate(pairs):
            copies.append(pltpu.make_async_copy(source, target, sems.at[i, k]))
    for copy in copies:
        copy.start()
    for i in range(8):
        side, d = divmod(i, 4)
        heads = (heads0, heads1)[side]
        for h in range(2):
            at = h * 256
            x[at : at + 256, i * 128 : (i + 1) * 128] = heads[h * 4 + d, :256]
            columns = slice(1024 + i * 64, 1024 + (i + 1) * 64)
            x[at : at + 128, columns] = heads[h * 4 + d, 256:, :64]
            x[at + 128 : at + 256, columns] = heads[h * 4 + d, 256:, 64:]
    for copy in copies:
        copy.wait()
    value = dot(x[...], w[...]) + residual[...].astype(jnp.float32)
    stream[...] = value
    mean = jnp.mean(value * value, axis=1, keepdims=True)
    normed_ref[...] = (value * lax.rsqrt(mean + EPSILON) * gain_ref[...]).astype(jnp.bfloat16)
    own = pl.ds(pl.multiple_of((own_x * 2 + own_c) * 64, 64), 64)
    stream_ref[...] = stream[own, :]


def mix(at, heads, fixed, gain):
    length, width = 512, fixed[0].shape[1]
    whole = pl.BlockSpec(memory_space=pltpu.VMEM)
    return pl.pallas_call(
        mix_kernel,
        in_specs=[pl.BlockSpec(memory_space=pltpu.SMEM)] + [whole] * 3 + [pl.BlockSpec(memory_space=pl.ANY)] * 8,
        out_specs=[whole, whole],
        out_shape=[
            jax.ShapeDtypeStruct((64, width), jnp.float32),
            jax.ShapeDtypeStruct((length, width), jnp.bfloat16),
        ],
        scratch_shapes=[
            pltpu.VMEM((1536, width), jnp.bfloat16),
            pltpu.VMEM((length, width), jnp.bfloat16),
            pltpu.VMEM((length, 1536), jnp.bfloat16),
            pltpu.VMEM((length, width), jnp.float32),
            pltpu.SemaphoreType.DMA((8, 3)),
        ],
        compiler_params=pltpu.CompilerParams(vmem_limit_bytes=60 * 2**20),
        cost_estimate=pl.CostEstimate(flops=33 * 10**8, transcendentals=0, bytes_accessed=12 * 10**6),
        name="mix",
    )(at, heads[0], heads[1], gain, *fixed)


def feed_kernel(at_ref, normed, weights, keep_ref, send_ref, up, down, hidden, sems):
    own_c, own_y = at_ref[1], at_ref[2]
    rows, width = normed.shape[1], up.shape[3]
    copies = [
        [
            pltpu.make_async_copy(
                weights.at[:, d, :, pl.ds(k * width, width)], target.at[:, (own_y - d) % 4], sems.at[k, d]
            )
            for d in range(4)
        ]
        for k, target in enumerate((up, down))
    ]
    for copy in copies[0] + copies[1]:
        copy.start()
    for copy in copies[0]:
        copy.wait()
    whole = jnp.maximum(dot(normed[...], up[...].reshape(rows, width)), 0.0)
    whole = (whole * whole).astype(jnp.bfloat16)
    for h in range(2):
        value = whole[h * 256 : (h + 1) * 256]
        for k in range(4):
            x, c = h * 2 + k // 2, k % 2
            target = (own_c + c) % 2 * 256 + x * 64
            hidden[pl.ds(pl.multiple_of(target, 64), 64), :] = value[k * 64 : (k + 1) * 64]
    for copy in copies[1]:
        copy.wait()
    out = dot(hidden[...], down[...].reshape(rows, width), NT).astype(jnp.bfloat16)
    keep_ref[...] = out[:256].reshape(keep_ref.shape)
    send_ref[...] = out[256:].reshape(send_ref.shape)


def feed(at, normed, weights):
    length, width = normed.shape
    whole = pl.BlockSpec(memory_space=pltpu.VMEM)
    shape = jax.ShapeDtypeStruct((4, 64, width), jnp.bfloat16)
    inner = weights.shape[3] // 2
    gathered = pltpu.VMEM(weights.shape[:3] + (inner,), jnp.bfloat16)
    return pl.pallas_call(
        feed_kernel,
        in_specs=[pl.BlockSpec(memory_space=pltpu.SMEM), whole, pl.BlockSpec(memory_space=pltpu.HBM)],
        out_specs=[whole, whole],
        out_shape=[shape, shape],
        scratch_shapes=[
            gathered,
            gathered,
            pltpu.VMEM((length, inner), jnp.bfloat16),
            pltpu.SemaphoreType.DMA((2, 4)),
        ],
        compiler_params=pltpu.CompilerParams(vmem_limit_bytes=60 * 2**20),
        cost_estimate=pl.CostEstimate(flops=44 * 10**8, transcendentals=0, bytes_accessed=14 * 10**6),
        name="feed",
    )(at, normed, weights)


def along(value, axis):
    return [value] + [shifted(value, axis, d) for d in (1, 2, 3)]


def body(
    residual,
    query_major,
    keys_major,
    values_major,
    query_minor,
    keys_minor,
    values_minor,
    lambda_major,
    lambda_minor,
    gain_major,
    gain_minor,
    output_major,
    output_minor,
    mixer_gain,
    up_weight,
    down_weight,
):
    z, y, x, c = (lax.axis_index(a) for a in ("z", "y", "x", "c"))
    minor = jnp.concatenate([keys_minor.T, values_minor.T], axis=0)
    kv = jnp.concatenate([keys_major, values_major], axis=1)
    kv = jnp.concatenate([kv, minor[:, :256], minor[:, 256:]], axis=0)
    kv = lax.all_gather(kv, "z")
    q = jnp.concatenate([query_major, query_minor], axis=1)
    half = q.shape[0] // 2
    late = mirrored(q[half:])
    q = jnp.concatenate([q[:half], late], axis=0)
    fixed = jnp.concatenate([output_major, output_minor, residual], axis=0)
    fixed = along(fixed, "x")
    q = lax.all_gather(q, "y")
    weights = jnp.concatenate([up_weight, down_weight.T], axis=1)
    weights = along(weights, "y")
    weights = lax.all_gather(jnp.stack(weights), "z")

    mirror = lax.axis_size("z") - 1 - z
    short_part = (z > mirror).astype(jnp.int32)
    short = attend(jnp.stack([y, short_part, jnp.minimum(z, mirror)]), q, kv)
    short = lax.all_to_all(short, "y", 0, 0, tiled=True)
    long = attend(jnp.stack([y, 1 - short_part, jnp.maximum(z, mirror)]), q, kv)
    long, *fixed = lax.optimization_barrier((long, *fixed))
    fixed = fixed + [shifted(f, "c", 1) for f in fixed]
    long = lax.all_to_all(long, "y", 0, 0, tiled=True)
    lams = jnp.concatenate([lambda_major, lambda_minor])
    early, late = merge(short_part[None], lams, gain_major[:, None], gain_minor[:, None], short, long)
    heads = jnp.stack(along(early, "x") + along(mirrored(late), "x"))
    heads = (heads, shifted(heads, "c", 1))
    at = jnp.stack([x, c, y]).astype(jnp.int32)
    stream, normed = mix(at, heads, fixed, mixer_gain[None])
    keep, send = feed(at, normed, weights)
    pair = keep.astype(jnp.float32) + shifted(send, "c", 1).astype(jnp.float32)
    blocks = lax.all_to_all(pair.astype(jnp.bfloat16), "x", 0, 0, tiled=True)
    return (stream + jnp.sum(blocks.astype(jnp.float32), axis=0)).astype(jnp.bfloat16)


def solution(mesh):
    finer = Mesh(mesh.devices.reshape(8, 4, 4, 2), ("z", "y", "x", "c"))
    placed = (
        P(SP + TP, None),
        P(SP, TP),
        P(SP, TP),
        P(SP, TP),
        P(SP, TP),
        P(SP, TP),
        P(SP, TP),
        P(TP),
        P(TP),
        P(),
        P(),
        P(TP, None),
        P(TP, None),
        P(),
        P(SP, TP),
        P(TP, SP),
    )

    return jax.shard_map(body, mesh=finer, in_specs=placed, out_specs=P(SP + TP, None), check_vma=False)
```
